32 devices in a mesh: grp: 1, ep: 32 (over z, y, x, core).
Axes of the slice: x: 2, y: 2, z: 4, core: 2. Of those that a mesh axis runs over, the one named last changes fastest.
Arguments:
- residual_input: bfloat16 [768, 2048], P(('grp', 'ep')), may hold values from -6 to 6
- attention_norm_gain: bfloat16 [2048], replicated, may hold values from 0.099609375 to 1.8984375
- receptance_weight: bfloat16 [2048, 1024], P(None, 'ep'), may hold values from -0.125 to 0.125
- key_weight: bfloat16 [2048, 1024], P(None, 'ep'), may hold values from -0.125 to 0.125
- value_weight: bfloat16 [2048, 1024], P(None, 'ep'), may hold values from -0.125 to 0.125
- decay_weight: bfloat16 [2048, 1024], P(None, 'ep'), may hold values from -0.125 to 0.125
- correction_rate_weight: bfloat16 [2048, 1024], P(None, 'ep'), may hold values from -0.125 to 0.125
- output_gate_weight: bfloat16 [2048, 1024], P(None, 'ep'), may hold values from -0.125 to 0.125
- decay_offset: float32 [1024], replicated, may hold values from -3 to 1
- correction_rate_offset: float32 [1024], replicated, may hold values from -1.5 to 1.5
- self_term_weight: float32 [1024], replicated, may hold values from -2 to 2
- head_read_gain: float32 [1024], replicated, may hold values from 0.1 to 1.9
- previous_state: float32 [768, 16, 4096], P(('grp', 'ep')), may hold values from -4 to 4
- attention_output_weight: bfloat16 [1024, 2048], replicated, may hold values from -0.1875 to 0.1875
- feedforward_norm_gain: bfloat16 [2048], replicated, may hold values from 0.099609375 to 1.8984375
- routes: int32 [768, 4], P('grp'), may hold values from 0 to 31, all different within a row; in each aligned block of 24 rows (0 to 23, 24 to 47, ...) at most 4 rows name the same one
- routing_weight: float32 [768, 4], P('grp'), may hold values from 0.2 to 1
- routed_gate_weight: bfloat16 [32, 2048, 512], P('ep'), may hold values from -0.125 to 0.125
- routed_up_weight: bfloat16 [32, 2048, 512], P('ep'), may hold values from -0.125 to 0.125
- routed_down_weight: bfloat16 [32, 512, 2048], P('ep'), may hold values from -0.25 to 0.25
- common_gate_weight: bfloat16 [2048, 512], replicated, may hold values from -0.125 to 0.125
- common_up_weight: bfloat16 [2048, 512], replicated, may hold values from -0.125 to 0.125
- common_down_weight: bfloat16 [512, 2048], replicated, may hold values from -0.25 to 0.25
Outputs:
- hidden_out: bfloat16 [768, 2048], P(('grp', 'ep'))
- next_state: float32 [768, 16, 4096], P(('grp', 'ep'))
The draws below stay inside these ranges and needn't reach their ends.
Inputs may be any that keep to these rules, and one draw needn't show every extreme that they name: `routes`: the 4 entries of a row differ. In each aligned block of 24 rows (the tokens of one index of ep) no expert is named by more than 4 rows, a bound that some block reaches.
All inputs are finite; a program needn't handle non-finite values.
Results may differ from the reference program's by a relative error of at most 0.013.
Values may be sent and summed in bfloat16 or wider, within the bound.
A program may use at most 128 MiB of HBM per device.

```python
import math
import jax
import jax.numpy as jnp
import numpy as np
from jax import lax

D = 2048
HEAD_COUNT = 16
HEAD_SIZE = 64
MIXER_WIDTH = 1024
EFF = 512
SFF = 512
EXPERTS = 32
TOPK = 4
CAP = 4
SEQ_DEV = 24
TOKENS = 768
N_EP = 32


def block_levels(key, shape, shards, least, high):
    level, own = 1.0, jax.random.fold_in(key, 6)
    for position, blocks in shards:
        heights = jnp.exp(jax.random.uniform(jax.random.fold_in(own, position), (blocks,), jnp.float32, least / len(shards), high / len(shards)))
        level = level * jnp.repeat(heights, shape[position] // blocks).reshape([-1 if axis == position else 1 for axis in range(len(shape))])
    return level


def routed_block(key, own, number, rows, amount, top, reach, skew):
    sequence = jax.random.permutation(key, amount)
    heavy_load, common = shares(amount, rows * top, reach, skew, True), shares(amount, rows * top, reach, skew, False)
    places = jnp.arange(amount)

    def named(tallies, turn):
        used = int((tallies > 0).sum())
        fixed = max(1, used // 4)
        passed = fixed + (places - fixed + turn * (used - fixed)) % max(1, amount - fixed)
        return jnp.zeros((amount,), jnp.int32).at[sequence[jnp.where(places < fixed, places, passed)]].set(jnp.asarray(tallies, jnp.int32))

    tallies = jnp.where(number % 4 == 0, named(heavy_load, number // 4), named(common, number - number // 4 - 1))
    mixed = jax.random.permutation(jax.random.fold_in(own, 3), amount)
    source_of, receiver = mixed[0:amount // 2 * 2:2], mixed[1:amount // 2 * 2:2]
    room = jnp.minimum(tallies[source_of] - 1, reach - tallies[receiver]) // 2
    room = jnp.where((source_of == sequence[0]) | (receiver == sequence[0]) | (tallies[receiver] == 0), 0, jnp.maximum(room, 0))
    passed = jax.random.randint(jax.random.fold_in(own, 4), (amount // 2,), 0, 1 << 20) % (room + 1)
    tallies = tallies.at[source_of].add(-passed).at[receiver].add(passed)
    members = jnp.searchsorted(jnp.cumsum(tallies), jnp.arange(rows * top), side="right").astype(jnp.int32)
    table = members.reshape(top, rows).T
    table = table[jax.random.permutation(jax.random.fold_in(own, 1), rows)]
    turn = jax.random.randint(jax.random.fold_in(own, 2), (rows, 1), 0, top)
    return jnp.take_along_axis(table, (jnp.arange(top)[None, :] + turn) % top, axis=1)


def shares(count, total, most, slope, full):
    loads = [(1 << 20) // math.isqrt(rank ** slope) + 1 for rank in range(1, count + 1)]
    largest = most if full else min(most, max(-(-total // count), total * loads[0] // sum(loads)))
    least = 1 if total - largest >= count - 1 else 0
    given, rest = [largest] + [least] * (count - 1), total - largest - least * (count - 1)
    while rest > 0:
        candidates = [i for i in range(1, count) if given[i] < largest] or [i for i in range(1, count) if given[i] < most]
        mass, remaining = sum([loads[i] for i in candidates]), rest
        for i in candidates:
            extra = min(most - given[i], max(1, remaining * loads[i] // mass), rest)
            given[i] = given[i] + extra
            rest = rest - extra
    return np.array(given)


def scatter_about(own_key, dims, scale, most, shards=(), kind=jnp.bfloat16):
    level = block_levels(own_key, dims, shards, -0.22, 0.18) if shards else 1.0
    drawn = jax.random.normal(own_key, dims, jnp.float32) * scale * level
    return jnp.minimum(jnp.maximum(drawn, -most), most).astype(kind)


def setup_inputs(seed: int = 0, part: int = 0) -> dict:
    splits = jax.random.split(jax.random.key(seed), 24)
    part_keys = jax.random.split(jax.random.fold_in(splits[23], part), 24)
    residual_input = scatter_about(part_keys[0], (TOKENS, D), 1.0, 6.0, ((0, 32),))
    attention_norm_gain = jnp.clip(1.0 + 0.18 * jax.random.normal(splits[1], (D,), jnp.float32), 0.099609375, 1.8984375).astype(jnp.bfloat16)
    receptance_weight = scatter_about(splits[2], (D, MIXER_WIDTH), D ** -0.5, 0.125, ((1, 32),))
    key_weight = scatter_about(splits[3], (D, MIXER_WIDTH), D ** -0.5, 0.125, ((1, 32),))
    value_weight = scatter_about(splits[4], (D, MIXER_WIDTH), D ** -0.5, 0.125, ((1, 32),))
    decay_weight = scatter_about(splits[5], (D, MIXER_WIDTH), D ** -0.5, 0.125, ((1, 32),))
    correction_rate_weight = scatter_about(splits[6], (D, MIXER_WIDTH), D ** -0.5, 0.125, ((1, 32),))
    output_gate_weight = scatter_about(splits[7], (D, MIXER_WIDTH), D ** -0.5, 0.125, ((1, 32),))
    decay_offset = jnp.clip(jax.random.uniform(splits[8], (MIXER_WIDTH,), jnp.float32, -3.0, 1.0), -3.0, 1.0)
    correction_rate_offset = jnp.clip(jax.random.uniform(splits[9], (MIXER_WIDTH,), jnp.float32, -1.5, 1.5), -1.5, 1.5)
    self_term_weight = scatter_about(splits[10], (MIXER_WIDTH,), 0.15, 2.0, (), jnp.float32)
    head_read_gain = jnp.clip(1.0 + 0.18 * jax.random.normal(splits[11], (MIXER_WIDTH,), jnp.float32), 0.1, 1.9)
    previous_state = scatter_about(part_keys[12], (TOKENS, HEAD_COUNT, HEAD_SIZE * HEAD_SIZE), 0.3, 4.0, ((0, 32),), jnp.float32)
    attention_output_weight = scatter_about(splits[13], (MIXER_WIDTH, D), MIXER_WIDTH ** -0.5, 0.1875)
    feedforward_norm_gain = jnp.clip(1.0 + 0.18 * jax.random.normal(splits[14], (D,), jnp.float32), 0.099609375, 1.8984375).astype(jnp.bfloat16)
    routes_keys = jax.random.split(jax.random.fold_in(part_keys[15], 1), TOKENS // SEQ_DEV)
    routes_turns = jax.random.permutation(jax.random.fold_in(part_keys[15], 3), TOKENS // SEQ_DEV)
    routes = jax.vmap(lambda own, number: routed_block(jax.random.fold_in(part_keys[15], 2), own, number, SEQ_DEV, EXPERTS, TOPK, CAP, 2))(routes_keys, routes_turns).reshape((TOKENS, TOPK))
    routing_weight = jnp.clip(jax.random.uniform(part_keys[16], (TOKENS, TOPK), jnp.float32, 0.2, 1.0), 0.2, 1.0)
    routed_gate_weight = scatter_about(splits[17], (EXPERTS, D, EFF), D ** -0.5, 0.125, ((0, 32),))
    routed_up_weight = scatter_about(splits[18], (EXPERTS, D, EFF), D ** -0.5, 0.125, ((0, 32),))
    routed_down_weight = scatter_about(splits[19], (EXPERTS, EFF, D), EFF ** -0.5, 0.25, ((0, 32),))
    common_gate_weight = scatter_about(splits[20], (D, SFF), D ** -0.5, 0.125)
    common_up_weight = scatter_about(splits[21], (D, SFF), D ** -0.5, 0.125)
    common_down_weight = scatter_about(splits[22], (SFF, D), SFF ** -0.5, 0.25)
    return {"residual_input": residual_input, "attention_norm_gain": attention_norm_gain, "receptance_weight": receptance_weight, "key_weight": key_weight, "value_weight": value_weight, "decay_weight": decay_weight, "correction_rate_weight": correction_rate_weight, "output_gate_weight": output_gate_weight, "decay_offset": decay_offset, "correction_rate_offset": correction_rate_offset, "self_term_weight": self_term_weight, "head_read_gain": head_read_gain, "previous_state": previous_state, "attention_output_weight": attention_output_weight, "feedforward_norm_gain": feedforward_norm_gain, "routes": routes, "routing_weight": routing_weight, "routed_gate_weight": routed_gate_weight, "routed_up_weight": routed_up_weight, "routed_down_weight": routed_down_weight, "common_gate_weight": common_gate_weight, "common_up_weight": common_up_weight, "common_down_weight": common_down_weight}


def rms_norm(value_rows, gain):
    scale = lax.rsqrt(lax.optimization_barrier(jnp.mean(value_rows * value_rows, axis=-1, keepdims=True)) + 1e-06)
    return (value_rows * scale * gain.astype(jnp.float32)).astype(jnp.bfloat16)

def expert_mlp(rows, gate_w, up_w, down_w):
    gate = jnp.dot(rows, gate_w, preferred_element_type=jnp.float32)
    upward = jnp.dot(rows, up_w, preferred_element_type=jnp.float32)
    hidden = (jax.nn.silu(gate) * upward).astype(jnp.bfloat16)
    return jnp.dot(hidden, down_w, preferred_element_type=jnp.float32).astype(jnp.bfloat16)

def attention_mixer(receptance_rows, key_rows, value_rows, decay_logit, rate_logit, gate_logit, decay_offset, correction_rate_offset, self_term_weight, head_read_gain, head_state):
    tally_value = receptance_rows.shape[0]

    def heads(tensor):
        return tensor.astype(jnp.float32).reshape(tally_value, HEAD_COUNT, HEAD_SIZE)
    decay = jnp.exp(-jnp.exp(-jax.nn.softplus(-(decay_offset + decay_logit.astype(jnp.float32))) - 0.5))
    rate = jax.nn.sigmoid(correction_rate_offset + rate_logit.astype(jnp.float32))
    key_head = heads(key_rows)
    rate_head = heads(rate)
    receptance_head = heads(receptance_rows)
    head_value = heads(value_rows)
    unit_key = key_head * lax.rsqrt(1.0 + lax.optimization_barrier(jnp.sum(key_head * key_head, axis=-1, keepdims=True)))
    rate_scaled_key = key_head * rate_head
    removal = unit_key * rate_head
    matrix = head_state.reshape(tally_value, HEAD_COUNT, HEAD_SIZE, HEAD_SIZE)
    recalled = jnp.einsum('nhvk,nhk->nhv', matrix, unit_key, precision=lax.Precision.HIGHEST)
    matrix = matrix * heads(decay)[:, :, None, :] - recalled[..., None] * removal[:, :, None, :] + head_value[..., None] * rate_scaled_key[:, :, None, :]
    read = jnp.einsum('nhvk,nhk->nhv', matrix, receptance_head, precision=lax.Precision.HIGHEST)
    centered = read - lax.optimization_barrier(jnp.mean(read, axis=-1, keepdims=True))
    variance = lax.optimization_barrier(jnp.mean(centered * centered, axis=-1, keepdims=True))
    normed_head_read = centered * lax.rsqrt(variance + 0.00064) * head_read_gain.reshape(HEAD_COUNT, HEAD_SIZE)
    self_term = lax.optimization_barrier(jnp.sum(receptance_head * rate_scaled_key * self_term_weight.reshape(HEAD_COUNT, HEAD_SIZE), axis=-1, keepdims=True)) * head_value
    normed_mixer_input = (normed_head_read + self_term).reshape(tally_value, HEAD_COUNT * HEAD_SIZE) * jax.nn.sigmoid(gate_logit.astype(jnp.float32))
    return (normed_mixer_input.astype(jnp.bfloat16), matrix.reshape(tally_value, HEAD_COUNT, HEAD_SIZE * HEAD_SIZE))

def routed_sum(normed_ffn, routes, routing_weight, routed_gate_weight, routed_up_weight, routed_down_weight):
    tokens = normed_ffn.shape[0]
    limit = N_EP * CAP
    slots = jnp.arange(limit, dtype=jnp.int32)

    def add_expert(expert_id, total):
        match = routes == expert_id
        hit = jnp.any(match, axis=1).astype(jnp.int32)
        weight = lax.optimization_barrier(jnp.sum(jnp.where(match, routing_weight, 0.0), axis=1))
        rank = jnp.cumsum(hit) - hit
        select = (rank[None, :] == slots[:, None]) & (hit[None, :] == 1)
        rows = jnp.dot(select.astype(jnp.bfloat16), normed_ffn, preferred_element_type=jnp.float32).astype(jnp.bfloat16)
        output = expert_mlp(rows, routed_gate_weight[expert_id], routed_up_weight[expert_id], routed_down_weight[expert_id])
        spread = select.astype(jnp.float32).T * weight[:, None]
        return total + jnp.dot(spread, output.astype(jnp.float32), precision=lax.Precision.HIGHEST)
    return lax.fori_loop(0, EXPERTS, add_expert, jnp.zeros((tokens, normed_ffn.shape[1]), jnp.float32))

def reference(residual_input, attention_norm_gain, receptance_weight, key_weight, value_weight, decay_weight, correction_rate_weight, output_gate_weight, decay_offset, correction_rate_offset, self_term_weight, head_read_gain, previous_state, attention_output_weight, feedforward_norm_gain, routes, routing_weight, routed_gate_weight, routed_up_weight, routed_down_weight, common_gate_weight, common_up_weight, common_down_weight):
    normed = rms_norm(residual_input.astype(jnp.float32), attention_norm_gain)

    def apply_projection(weight):
        return jnp.dot(normed, weight, preferred_element_type=jnp.float32).astype(jnp.bfloat16)
    normed_mixer_input, next_state = attention_mixer(apply_projection(receptance_weight), apply_projection(key_weight), apply_projection(value_weight), apply_projection(decay_weight), apply_projection(correction_rate_weight), apply_projection(output_gate_weight), decay_offset, correction_rate_offset, self_term_weight, head_read_gain, previous_state)
    attended = jnp.dot(normed_mixer_input, attention_output_weight, preferred_element_type=jnp.float32).astype(jnp.bfloat16)
    middle = residual_input.astype(jnp.float32) + attended.astype(jnp.float32)
    normed_ffn = rms_norm(middle, feedforward_norm_gain)
    shared = expert_mlp(normed_ffn, common_gate_weight, common_up_weight, common_down_weight)
    routed = routed_sum(normed_ffn, routes, routing_weight, routed_gate_weight, routed_up_weight, routed_down_weight)
    hidden_out = (middle + shared.astype(jnp.float32) + routed).astype(jnp.bfloat16)
    return (hidden_out, next_state)
```

```python
import functools
import math

import jax
import jax.numpy as jnp
import numpy as np
from jax import lax
from jax.experimental import pallas as pl
from jax.experimental.pallas import tpu as pltpu
from jax.sharding import PartitionSpec as P

HEAD_COUNT = 16
HEAD_SIZE = 64
CAP = 4
ROLES = 6
LANES = 128
F32 = jnp.float32
BF16 = jnp.bfloat16


def rms_norm(value_rows, gain):
    scale = lax.rsqrt(jnp.mean(value_rows * value_rows, axis=-1, keepdims=True) + 1e-06)
    return (value_rows * scale * gain.astype(F32)).astype(BF16)


def expert_mlp(rows, gate_w, up_w, down_w):
    gate = jnp.dot(rows, gate_w, preferred_element_type=F32)
    upward = jnp.dot(rows, up_w, preferred_element_type=F32)
    hidden = (jax.nn.silu(gate) * upward).astype(BF16)
    return jnp.dot(hidden, down_w, preferred_element_type=F32).astype(BF16)


def place_matrices(pieces):
    width = HEAD_SIZE // pieces
    place = np.zeros((pieces, ROLES * width, ROLES * LANES), np.float32)
    for piece in range(pieces):
        for role in range(ROLES):
            for column in range(width):
                for copy in range(LANES // HEAD_SIZE):
                    lane = role * LANES + copy * HEAD_SIZE + piece * width + column
                    place[piece, role * width + column, lane] = 1.0
    return place


def split(value):
    high = value.astype(BF16)
    return high, (value - high.astype(F32)).astype(BF16)


def dot(a, b):
    return jnp.dot(a, b, preferred_element_type=F32)


def mixer_kernel(
    land_ref, place_ref, spread_ref, gather_ref, block_ref, consts_ref, state_ref, out_w_ref,
    resid_ref, gain_ref, select_ref,
    next_ref, middle_ref, normed_ref, rows_ref,
    role_ref, mixed_ref,
):
    step = pl.program_id(0)
    tokens = land_ref.shape[1]
    pieces = place_ref.shape[0]
    step_rows = state_ref.shape[0] * HEAD_COUNT

    @pl.when(step == 0)
    def _():
        for head in range(HEAD_COUNT):
            total = dot(land_ref[head * pieces], place_ref[0])
            for piece in range(1, pieces):
                total = total + dot(land_ref[head * pieces + piece], place_ref[piece])
            for number in range(ROLES):
                part = total[:, number * LANES : (number + 1) * LANES]
                role_ref[number, pl.ds(head, tokens, stride=HEAD_COUNT), :] = part

    base = pl.multiple_of(step * step_rows, step_rows)

    def role(number):
        return role_ref[number, pl.ds(base, step_rows), :]

    def const(number):
        one = consts_ref[number]
        return jnp.concatenate([one] * state_ref.shape[0], axis=0)

    half = HEAD_SIZE / LANES

    def head_sum(value):
        return jnp.sum(value, axis=-1, keepdims=True) * half

    receptance, keys, values = role(0), role(1), role(2)
    decay = jnp.exp(-math.exp(-0.5) * jax.nn.sigmoid(const(0) + role(3)))
    rate = jax.nn.sigmoid(const(1) + role(4))
    unit_key = keys * lax.rsqrt(1.0 + head_sum(keys * keys))
    scaled_key = keys * rate
    removal = unit_key * rate
    self_sum = head_sum(receptance * scaled_key * const(2))

    def twice(value):
        return jnp.concatenate([value, value], axis=1)

    unit_key2, decay2, removal2 = twice(unit_key), twice(decay), twice(removal)
    scaled_key2, receptance2 = twice(scaled_key), twice(receptance)
    values_b = values[:, :HEAD_SIZE].astype(BF16)
    block = block_ref[...]
    chunk = block.shape[0]
    read = jnp.zeros((step_rows, LANES), F32)
    group = state_ref.shape[0]
    for c in range(HEAD_SIZE * HEAD_SIZE // chunk):
        cols = slice(c * chunk, (c + 1) * chunk)
        state = state_ref[:, :, cols].reshape(step_rows, chunk)
        high, low = split(state * unit_key2)
        recalled = dot(high, block) + dot(low, block)
        spread = dot(values_b, spread_ref[:, cols])
        new = state * decay2 - recalled * removal2 + spread * scaled_key2
        next_ref[:, :, cols] = new.reshape(group, HEAD_COUNT, chunk)
        high, low = split(new * receptance2)
        pick = gather_ref[cols, :]
        read = read + dot(high, pick) + dot(low, pick)
    centered = read - head_sum(read) * (1.0 / HEAD_SIZE)
    variance = head_sum(centered * centered) * (1.0 / HEAD_SIZE)
    normal = centered * lax.rsqrt(variance + 0.00064) * const(3)
    mixed_ref[pl.ds(base, step_rows), :] = (normal + self_sum * values) * jax.nn.sigmoid(role(5))

    @pl.when(step == pl.num_programs(0) - 1)
    def _():
        lane = lax.broadcasted_iota(jnp.int32, (tokens, LANES), 1)
        per = LANES // HEAD_SIZE
        parts = []
        for first in range(0, HEAD_COUNT, per):
            part = mixed_ref[pl.ds(first, tokens, stride=HEAD_COUNT), :]
            for other in range(1, per):
                rest = mixed_ref[pl.ds(first + other, tokens, stride=HEAD_COUNT), :]
                part = jnp.where(lane < other * HEAD_SIZE, part, rest)
            parts.append(part.astype(BF16))
        mixed = jnp.concatenate(parts, axis=1)
        attended = dot(mixed, out_w_ref[...]).astype(BF16).astype(F32)
        middle = resid_ref[...].astype(F32) + attended
        middle_ref[...] = middle
        normed = rms_norm(middle, gain_ref[...])
        normed_ref[...] = normed
        rows_ref[...] = dot(select_ref[...], normed).astype(BF16)


def mixer(land, consts, state, out_w, resid, gain, select):
    sources, tokens, width = land.shape
    pieces = sources // HEAD_COUNT
    model = resid.shape[1]
    group = 8 if tokens % 8 == 0 else 1
    chunk = 4 * HEAD_SIZE
    place = jnp.asarray(place_matrices(pieces), BF16)
    eye = np.eye(HEAD_SIZE, dtype=np.float32)
    spread = jnp.asarray(np.repeat(eye, HEAD_SIZE, axis=1), BF16)
    gather = jnp.asarray(np.repeat(np.concatenate([eye] * (LANES // HEAD_SIZE), 1), HEAD_SIZE, 0), BF16)
    block = jnp.asarray(np.kron(np.eye(chunk // HEAD_SIZE), np.ones((HEAD_SIZE, HEAD_SIZE))), BF16)
    full = lambda array: pl.BlockSpec(array.shape, lambda i: (0,) * array.ndim)
    state_spec = pl.BlockSpec((group,) + state.shape[1:], lambda i: (i, 0, 0))
    operands = (land, place, spread, gather, block, consts, state, out_w, resid, gain, select)
    specs = [full(a) for a in operands]
    specs[6] = state_spec
    whole = lambda shape: pl.BlockSpec(shape, lambda i: (0,) * len(shape))
    slots = select.shape[0]
    return pl.pallas_call(
        mixer_kernel,
        grid=(tokens // group,),
        out_shape=(
            jax.ShapeDtypeStruct(state.shape, F32),
            jax.ShapeDtypeStruct((tokens, model), F32),
            jax.ShapeDtypeStruct((tokens, model), BF16),
            jax.ShapeDtypeStruct((slots, model), BF16),
        ),
        in_specs=specs,
        out_specs=(state_spec, whole((tokens, model)), whole((tokens, model)), whole((slots, model))),
        scratch_shapes=[
            pltpu.VMEM((ROLES, tokens * HEAD_COUNT, LANES), F32),
            pltpu.VMEM((tokens * HEAD_COUNT, LANES), F32),
        ],
        compiler_params=pltpu.CompilerParams(vmem_limit_bytes=50 * 1024 * 1024),
        cost_estimate=pl.CostEstimate(flops=4_000_000_000, bytes_accessed=20_000_000, transcendentals=0),
    )(*operands)


def per_device(
    residual_input,
    attention_norm_gain,
    receptance_weight,
    key_weight,
    value_weight,
    decay_weight,
    correction_rate_weight,
    output_gate_weight,
    decay_offset,
    correction_rate_offset,
    self_term_weight,
    head_read_gain,
    previous_state,
    attention_output_weight,
    feedforward_norm_gain,
    routes,
    routing_weight,
    routed_gate_weight,
    routed_up_weight,
    routed_down_weight,
    common_gate_weight,
    common_up_weight,
    common_down_weight,
):
    ep_size = lax.axis_size("ep")
    device = lax.axis_index("ep")
    tokens, model = residual_input.shape
    normed = rms_norm(residual_input.astype(F32), attention_norm_gain)
    stacked = jnp.concatenate(
        (
            receptance_weight,
            key_weight,
            value_weight,
            decay_weight,
            correction_rate_weight,
            output_gate_weight,
        ),
        axis=1,
    )
    own_routes = lax.dynamic_slice_in_dim(routes, device * tokens, tokens, 0)
    own_weight = lax.dynamic_slice_in_dim(routing_weight, device * tokens, tokens, 0)
    experts = routed_gate_weight.shape[0] * ep_size
    match = own_routes[:, :, None] == jnp.arange(experts, dtype=jnp.int32)
    hit = jnp.any(match, axis=1)
    weight = jnp.sum(jnp.where(match, own_weight[:, :, None], 0.0), axis=1)
    rank = jnp.cumsum(hit.astype(jnp.int32), axis=0) - hit.astype(jnp.int32)
    chosen = hit[:, :, None] & (rank[:, :, None] == jnp.arange(CAP, dtype=jnp.int32))
    select = chosen.astype(BF16).reshape(tokens, experts * CAP)
    coefficient = jnp.where(chosen, weight[:, :, None], 0.0).reshape(tokens, experts * CAP)
    coef_high, coef_low = split(coefficient)

    cols = dot(lax.all_gather(normed, "ep", axis=0, tiled=True), stacked).astype(BF16)
    land = lax.all_to_all(
        cols.reshape(ep_size, tokens, cols.shape[-1]), "ep", split_axis=0, concat_axis=0, tiled=True
    )
    by_head = jnp.stack((decay_offset, correction_rate_offset, self_term_weight, head_read_gain))
    by_head = by_head.reshape(4, HEAD_COUNT, HEAD_SIZE)
    consts = jnp.concatenate([by_head] * (LANES // HEAD_SIZE), axis=-1)
    next_state, middle, normed_ffn, rows = mixer(
        land,
        consts,
        previous_state,
        attention_output_weight,
        residual_input,
        feedforward_norm_gain.reshape(1, model),
        select.T,
    )
    served = lax.all_to_all(
        rows.reshape(ep_size, -1, model), "ep", split_axis=0, concat_axis=0, tiled=True
    )
    shared = expert_mlp(normed_ffn, common_gate_weight, common_up_weight, common_down_weight)
    output = expert_mlp(
        served.reshape(-1, model),
        routed_gate_weight[0],
        routed_up_weight[0],
        routed_down_weight[0],
    )
    returned = lax.all_to_all(
        output.reshape(ep_size, -1, model), "ep", split_axis=0, concat_axis=0, tiled=True
    ).reshape(-1, model)
    routed = dot(
        jnp.concatenate((coef_high, coef_low), axis=0), returned
    )
    routed = routed[:tokens] + routed[tokens:]
    hidden_out = (middle + shared.astype(F32) + routed).astype(BF16)
    return (hidden_out, next_state)


def solution(mesh):
    return jax.shard_map(
        per_device,
        mesh=mesh,
        in_specs=(
            P(("grp", "ep"), None),
            P(),
            P(None, "ep"),
            P(None, "ep"),
            P(None, "ep"),
            P(None, "ep"),
            P(None, "ep"),
            P(None, "ep"),
            P(),
            P(),
            P(),
            P(),
            P(("grp", "ep"), None, None),
            P(),
            P(),
            P("grp", None),
            P("grp", None),
            P("ep", None, None),
            P("ep", None, None),
            P("ep", None, None),
            P(),
            P(),
            P(),
        ),
        out_specs=(P(("grp", "ep"), None), P(("grp", "ep"), None, None)),
        check_vma=False,
    )
```

```python
import functools
import math

import jax
import jax.numpy as jnp
import numpy as np
from jax import lax
from jax.experimental import pallas as pl
from jax.experimental.pallas import tpu as pltpu
from jax.sharding import PartitionSpec as P

HEAD_COUNT = 16
HEAD_SIZE = 64
CAP = 4
ROLES = 6
LANES = 128
F32 = jnp.float32
BF16 = jnp.bfloat16


def rms_norm(value_rows, gain):
    scale = lax.rsqrt(jnp.mean(value_rows * value_rows, axis=-1, keepdims=True) + 1e-06)
    return (value_rows * scale * gain.astype(F32)).astype(BF16)


def expert_mlp(rows, gate_w, up_w, down_w):
    gate = jnp.dot(rows, gate_w, preferred_element_type=F32)
    upward = jnp.dot(rows, up_w, preferred_element_type=F32)
    hidden = (jax.nn.silu(gate) * upward).astype(BF16)
    return jnp.dot(hidden, down_w, preferred_element_type=F32).astype(BF16)


def place_matrices(pieces):
    width = HEAD_SIZE // pieces
    place = np.zeros((pieces, ROLES * width, ROLES * LANES), np.float32)
    for piece in range(pieces):
        for role in range(ROLES):
            for column in range(width):
                for copy in range(LANES // HEAD_SIZE):
                    lane = role * LANES + copy * HEAD_SIZE + piece * width + column
                    place[piece, role * width + column, lane] = 1.0
    return place


def split(value):
    high = value.astype(BF16)
    return high, (value - high.astype(F32)).astype(BF16)


def dot(a, b):
    return jnp.dot(a, b, preferred_element_type=F32)


def mixer_kernel(
    land_ref, place_ref, spread_ref, gather_ref, block_ref, consts_ref, state_ref, out_w_ref,
    resid_ref, gain_ref, select_ref,
    next_ref, middle_ref, normed_ref, rows_ref,
    role_ref, mixed_ref,
):
    step = pl.program_id(0)
    tokens = land_ref.shape[1]
    pieces = place_ref.shape[0]
    step_rows = state_ref.shape[0] * HEAD_COUNT

    @pl.when(step == 0)
    def _():
        for head in range(HEAD_COUNT):
            total = dot(land_ref[head * pieces], place_ref[0])
            for piece in range(1, pieces):
                total = total + dot(land_ref[head * pieces + piece], place_ref[piece])
            for number in range(ROLES):
                part = total[:, number * LANES : (number + 1) * LANES]
                role_ref[number, pl.ds(head, tokens, stride=HEAD_COUNT), :] = part

    base = pl.multiple_of(step * step_rows, step_rows)

    def role(number):
        return role_ref[number, pl.ds(base, step_rows), :]

    def const(number):
        one = consts_ref[number]
        return jnp.concatenate([one] * state_ref.shape[0], axis=0)

    half = HEAD_SIZE / LANES

    def head_sum(value):
        return jnp.sum(value, axis=-1, keepdims=True) * half

    receptance, keys, values = role(0), role(1), role(2)
    decay = jnp.exp(-math.exp(-0.5) * jax.nn.sigmoid(const(0) + role(3)))
    rate = jax.nn.sigmoid(const(1) + role(4))
    unit_key = keys * lax.rsqrt(1.0 + head_sum(keys * keys))
    scaled_key = keys * rate
    removal = unit_key * rate
    self_sum = head_sum(receptance * scaled_key * const(2))

    def twice(value):
        return jnp.concatenate([value, value], axis=1)

    unit_key2, decay2, removal2 = twice(unit_key), twice(decay), twice(removal)
    scaled_key2, receptance2 = twice(scaled_key), twice(receptance)
    values_b = values[:, :HEAD_SIZE].astype(BF16)
    block = block_ref[...]
    chunk = block.shape[0]
    read = jnp.zeros((step_rows, LANES), F32)
    group = state_ref.shape[0]
    for c in range(HEAD_SIZE * HEAD_SIZE // chunk):
        cols = slice(c * chunk, (c + 1) * chunk)
        state = state_ref[:, :, cols].reshape(step_rows, chunk)
        high, low = split(state * unit_key2)
        recalled = dot(high, block) + dot(low, block)
        spread = dot(values_b, spread_ref[:, cols])
        new = state * decay2 - recalled * removal2 + spread * scaled_key2
        next_ref[:, :, cols] = new.reshape(group, HEAD_COUNT, chunk)
        high, low = split(new * receptance2)
        pick = gather_ref[cols, :]
        read = read + dot(high, pick) + dot(low, pick)
    centered = read - head_sum(read) * (1.0 / HEAD_SIZE)
    variance = head_sum(centered * centered) * (1.0 / HEAD_SIZE)
    normal = centered * lax.rsqrt(variance + 0.00064) * const(3)
    mixed_ref[pl.ds(base, step_rows), :] = (normal + self_sum * values) * jax.nn.sigmoid(role(5))

    @pl.when(step == pl.num_programs(0) - 1)
    def _():
        lane = lax.broadcasted_iota(jnp.int32, (tokens, LANES), 1)
        per = LANES // HEAD_SIZE
        parts = []
        for first in range(0, HEAD_COUNT, per):
            part = mixed_ref[pl.ds(first, tokens, stride=HEAD_COUNT), :]
            for other in range(1, per):
                rest = mixed_ref[pl.ds(first + other, tokens, stride=HEAD_COUNT), :]
                part = jnp.where(lane < other * HEAD_SIZE, part, rest)
            parts.append(part.astype(BF16))
        mixed = jnp.concatenate(parts, axis=1)
        attended = dot(mixed, out_w_ref[...]).astype(BF16).astype(F32)
        middle = resid_ref[...].astype(F32) + attended
        middle_ref[...] = middle
        normed = rms_norm(middle, gain_ref[...])
        normed_ref[...] = normed
        rows_ref[...] = dot(select_ref[...], normed).astype(BF16)


def mixer(land, consts, state, out_w, resid, gain, select):
    sources, tokens, width = land.shape
    pieces = sources // HEAD_COUNT
    model = resid.shape[1]
    group = 8 if tokens % 8 == 0 else 1
    chunk = 4 * HEAD_SIZE
    place = jnp.asarray(place_matrices(pieces), BF16)
    eye = np.eye(HEAD_SIZE, dtype=np.float32)
    spread = jnp.asarray(np.repeat(eye, HEAD_SIZE, axis=1), BF16)
    gather = jnp.asarray(np.repeat(np.concatenate([eye] * (LANES // HEAD_SIZE), 1), HEAD_SIZE, 0), BF16)
    block = jnp.asarray(np.kron(np.eye(chunk // HEAD_SIZE), np.ones((HEAD_SIZE, HEAD_SIZE))), BF16)
    full = lambda array: pl.BlockSpec(array.shape, lambda i: (0,) * array.ndim)
    state_spec = pl.BlockSpec((group,) + state.shape[1:], lambda i: (i, 0, 0))
    operands = (land, place, spread, gather, block, consts, state, out_w, resid, gain, select)
    specs = [full(a) for a in operands]
    specs[6] = state_spec
    whole = lambda shape: pl.BlockSpec(shape, lambda i: (0,) * len(shape))
    slots = select.shape[0]
    return pl.pallas_call(
        mixer_kernel,
        grid=(tokens // group,),
        out_shape=(
            jax.ShapeDtypeStruct(state.shape, F32),
            jax.ShapeDtypeStruct((tokens, model), F32),
            jax.ShapeDtypeStruct((tokens, model), BF16),
            jax.ShapeDtypeStruct((slots, model), BF16),
        ),
        in_specs=specs,
        out_specs=(state_spec, whole((tokens, model)), whole((tokens, model)), whole((slots, model))),
        scratch_shapes=[
            pltpu.VMEM((ROLES, tokens * HEAD_COUNT, LANES), F32),
            pltpu.VMEM((tokens * HEAD_COUNT, LANES), F32),
        ],
        compiler_params=pltpu.CompilerParams(vmem_limit_bytes=50 * 1024 * 1024),
        cost_estimate=pl.CostEstimate(flops=4_000_000_000, bytes_accessed=20_000_000, transcendentals=0),
    )(*operands)


PLANE = 8


def project_kernel(
    depth, normed_ref, w0, w1, w2, w3, w4, w5, land_out,
    weight_ref, held, cols, land,
    z_send, z_recv, near_send, near_recv, half_send, half_recv, core_send, core_recv,
    out_send, out_recv,
):
    total = depth * PLANE
    tokens, model = normed_ref.shape
    cut = model // 2
    me = lax.axis_index("ep")
    core = lax.rem(me, 2)
    x = lax.rem(me // 2, 2)
    y = lax.rem(me // 4, 2)
    along_x = me + 2 - 4 * x
    along_y = me + 4 - 8 * y
    mate = me + 1 - 2 * core
    plane = lax.rem(me, PLANE)
    plane_x, plane_y, plane_c = lax.rem(along_x, PLANE), lax.rem(along_y, PLANE), lax.rem(mate, PLANE)
    far = lax.rem(along_x + 4 - 8 * y, PLANE)
    level = me // PLANE

    def send(source, target, device, send_sem, recv_sem):
        copy = pltpu.make_async_remote_copy(
            src_ref=source, dst_ref=target, send_sem=send_sem, recv_sem=recv_sem,
            device_id={"ep": device}, device_id_type=pl.DeviceIdType.MESH,
        )
        copy.start()
        return copy

    def slot(of_plane, d):
        return held.at[of_plane, lax.rem(level + depth - d, depth)]

    sent = []
    along_z = [None]
    for d in range(1, depth):
        there = lax.rem(me + PLANE * d, total)
        along_z.append(send(normed_ref, slot(plane, 0), there, z_send.at[d], z_recv.at[d]))
    by_y, by_x, by_core = [], [], [[], [], [], []]
    for d in range(depth):
        if d:
            along_z[d].wait_recv()
        source = normed_ref if d == 0 else slot(plane, d)
        here = slot(plane, d)
        by_y.append(send(source, here, along_y, near_send.at[0, d], near_recv.at[0, d]))
        by_x.append(send(source, here, along_x, near_send.at[1, d], near_recv.at[1, d]))
        by_core[0].append(send(source, here, mate, core_send.at[0, d], core_recv.at[0, d]))
        if d == 0:
            held[plane, level] = normed_ref[...]
            weight_ref[...] = jnp.concatenate(
                [w[...] for w in (w0, w1, w2, w3, w4, w5)], axis=1
            )

    def compute(group):
        rows = held[group].astype(F32).reshape(depth * tokens, model).astype(BF16)
        result = dot(rows, weight_ref[...]).astype(BF16).astype(F32)
        cols[group] = result.reshape(depth, tokens, result.shape[-1]).astype(BF16)

    def give(group):
        for z in range(depth):
            to = z * PLANE + group
            number = lax.rem(to - me + total, total)

            @pl.when(to != me)
            def _():
                send(cols.at[group, z], land.at[me], to, out_send.at[number], out_recv.at[number])

            @pl.when(to == me)
            def _():
                land[me] = cols[group, z]

    compute(plane)
    halves = []
    for d in range(depth):
        by_y[d].wait_recv()
        block = held.at[plane_y, lax.rem(level + depth - d, depth)]
        first = block.at[:, :cut]
        halves.append(send(first, first, along_x, half_send.at[0, d], half_recv.at[0, d]))
        by_core[1].append(send(block, block, mate, core_send.at[1, d], core_recv.at[1, d]))
        by_x[d].wait_recv()
        block = held.at[plane_x, lax.rem(level + depth - d, depth)]
        second = block.at[:, cut:]
        halves.append(send(second, second, along_y, half_send.at[1, d], half_recv.at[1, d]))
        by_core[2].append(send(block, block, mate, core_send.at[2, d], core_recv.at[2, d]))
    compute(plane_y)
    give(plane)
    compute(plane_x)
    give(plane_y)
    for d in range(depth):
        halves[2 * d].wait_recv()
        halves[2 * d + 1].wait_recv()
        block = slot(far, d)
        by_core[3].append(send(block, block, mate, core_send.at[3, d], core_recv.at[3, d]))
    before = plane_x
    compute(far)
    give(before)
    before = far
    for which, group in enumerate((plane, plane_y, plane_x, far)):
        for d in range(depth):
            by_core[which][d].wait_recv()
        other = group + 1 - 2 * core
        compute(other)
        give(before)
        before = other
    give(before)
    for copy in along_z[1:] + by_y + by_x + halves + by_core[0] + by_core[1] + by_core[2] + by_core[3]:
        copy.wait_send()

    def finish(number, carry):
        copy = pltpu.make_async_remote_copy(
            src_ref=cols.at[0, 0], dst_ref=land.at[0],
            send_sem=out_send.at[number], recv_sem=out_recv.at[number],
            device_id={"ep": lax.rem(me + number, total)}, device_id_type=pl.DeviceIdType.MESH,
        )
        copy.wait_recv()
        copy.wait_send()
        return carry

    lax.fori_loop(1, total, finish, 0)
    land_out[...] = land[...]


def project(normed, weights, ep_size):
    depth = ep_size // PLANE
    tokens, model = normed.shape
    width = sum(w.shape[1] for w in weights)
    dma = pltpu.SemaphoreType.DMA
    return pl.pallas_call(
        functools.partial(project_kernel, depth),
        out_shape=jax.ShapeDtypeStruct((ep_size, tokens, width), BF16),
        in_specs=[pl.BlockSpec(memory_space=pltpu.VMEM)] * 7,
        out_specs=pl.BlockSpec(memory_space=pltpu.VMEM),
        scratch_shapes=[
            pltpu.VMEM((model, width), BF16),
            pltpu.VMEM((PLANE, depth, tokens, model), BF16),
            pltpu.VMEM((PLANE, depth, tokens, width), BF16),
            pltpu.VMEM((ep_size, tokens, width), BF16),
            dma((depth,)), dma((depth,)),
            dma((2, depth)), dma((2, depth)),
            dma((2, depth)), dma((2, depth)),
            dma((4, depth)), dma((4, depth)),
            dma((ep_size,)), dma((ep_size,)),
        ],
        compiler_params=pltpu.CompilerParams(
            has_side_effects=True, vmem_limit_bytes=40 * 1024 * 1024
        ),
        cost_estimate=pl.CostEstimate(flops=600_000_000, bytes_accessed=100_000_000, transcendentals=0),
    )(normed, *weights)


def per_device(
    residual_input,
    attention_norm_gain,
    receptance_weight,
    key_weight,
    value_weight,
    decay_weight,
    correction_rate_weight,
    output_gate_weight,
    decay_offset,
    correction_rate_offset,
    self_term_weight,
    head_read_gain,
    previous_state,
    attention_output_weight,
    feedforward_norm_gain,
    routes,
    routing_weight,
    routed_gate_weight,
    routed_up_weight,
    routed_down_weight,
    common_gate_weight,
    common_up_weight,
    common_down_weight,
):
    ep_size = lax.axis_size("ep")
    device = lax.axis_index("ep")
    tokens, model = residual_input.shape
    normed = rms_norm(residual_input.astype(F32), attention_norm_gain)
    own_routes = lax.dynamic_slice_in_dim(routes, device * tokens, tokens, 0)
    own_weight = lax.dynamic_slice_in_dim(routing_weight, device * tokens, tokens, 0)
    experts = routed_gate_weight.shape[0] * ep_size
    match = own_routes[:, :, None] == jnp.arange(experts, dtype=jnp.int32)
    hit = jnp.any(match, axis=1)
    weight = jnp.sum(jnp.where(match, own_weight[:, :, None], 0.0), axis=1)
    rank = jnp.cumsum(hit.astype(jnp.int32), axis=0) - hit.astype(jnp.int32)
    chosen = hit[:, :, None] & (rank[:, :, None] == jnp.arange(CAP, dtype=jnp.int32))
    select = chosen.astype(BF16).reshape(tokens, experts * CAP)
    coefficient = jnp.where(chosen, weight[:, :, None], 0.0).reshape(tokens, experts * CAP)
    coef_high, coef_low = split(coefficient)

    land = project(
        normed,
        (
            receptance_weight,
            key_weight,
            value_weight,
            decay_weight,
            correction_rate_weight,
            output_gate_weight,
        ),
        ep_size,
    )
    by_head = jnp.stack((decay_offset, correction_rate_offset, self_term_weight, head_read_gain))
    by_head = by_head.reshape(4, HEAD_COUNT, HEAD_SIZE)
    consts = jnp.concatenate([by_head] * (LANES // HEAD_SIZE), axis=-1)
    next_state, middle, normed_ffn, rows = mixer(
        land,
        consts,
        previous_state,
        attention_output_weight,
        residual_input,
        feedforward_norm_gain.reshape(1, model),
        select.T,
    )
    served = lax.all_to_all(
        rows.reshape(ep_size, -1, model), "ep", split_axis=0, concat_axis=0, tiled=True
    )
    shared = expert_mlp(normed_ffn, common_gate_weight, common_up_weight, common_down_weight)
    output = expert_mlp(
        served.reshape(-1, model),
        routed_gate_weight[0],
        routed_up_weight[0],
        routed_down_weight[0],
    )
    returned = lax.all_to_all(
        output.reshape(ep_size, -1, model), "ep", split_axis=0, concat_axis=0, tiled=True
    ).reshape(-1, model)
    routed = dot(
        jnp.concatenate((coef_high, coef_low), axis=0), returned
    )
    routed = routed[:tokens] + routed[tokens:]
    hidden_out = (middle + shared.astype(F32) + routed).astype(BF16)
    return (hidden_out, next_state)


def solution(mesh):
    return jax.shard_map(
        per_device,
        mesh=mesh,
        in_specs=(
            P(("grp", "ep"), None),
            P(),
            P(None, "ep"),
            P(None, "ep"),
            P(None, "ep"),
            P(None, "ep"),
            P(None, "ep"),
            P(None, "ep"),
            P(),
            P(),
            P(),
            P(),
            P(("grp", "ep"), None, None),
            P(),
            P(),
            P("grp", None),
            P("grp", None),
            P("ep", None, None),
            P("ep", None, None),
            P("ep", None, None),
            P(),
            P(),
            P(),
        ),
        out_specs=(P(("grp", "ep"), None), P(("grp", "ep"), None, None)),
        check_vma=False,
    )
```

```python
import functools
import math

import jax
import jax.numpy as jnp
import numpy as np
from jax import lax
from jax.experimental import pallas as pl
from jax.experimental.pallas import tpu as pltpu
from jax.sharding import PartitionSpec as P

HEAD_COUNT = 16
HEAD_SIZE = 64
CAP = 4
ROLES = 6
LANES = 128
F32 = jnp.float32
BF16 = jnp.bfloat16


def rms_norm(value_rows, gain):
    scale = lax.rsqrt(jnp.mean(value_rows * value_rows, axis=-1, keepdims=True) + 1e-06)
    return (value_rows * scale * gain.astype(F32)).astype(BF16)


def expert_mlp(rows, gate_w, up_w, down_w):
    gate = jnp.dot(rows, gate_w, preferred_element_type=F32)
    upward = jnp.dot(rows, up_w, preferred_element_type=F32)
    hidden = (jax.nn.silu(gate) * upward).astype(BF16)
    return jnp.dot(hidden, down_w, preferred_element_type=F32).astype(BF16)


def place_matrices(pieces):
    width = HEAD_SIZE // pieces
    place = np.zeros((pieces, ROLES * width, ROLES * LANES), np.float32)
    for piece in range(pieces):
        for role in range(ROLES):
            for column in range(width):
                for copy in range(LANES // HEAD_SIZE):
                    lane = role * LANES + copy * HEAD_SIZE + piece * width + column
                    place[piece, role * width + column, lane] = 1.0
    return place


def split(value):
    high = value.astype(BF16)
    return high, (value - high.astype(F32)).astype(BF16)


def dot(a, b):
    return jnp.dot(a, b, preferred_element_type=F32)


def mixer_kernel(
    land_ref, place_ref, spread_ref, gather_ref, block_ref, const0, const1, const2, const3, state_ref, out_w_ref,
    resid_ref, gain_ref, select_ref,
    next_ref, middle_ref, normed_ref, rows_ref,
    role_ref, mixed_ref, consts_ref,
):
    step = pl.program_id(0)
    tokens = land_ref.shape[1]
    pieces = place_ref.shape[0]
    step_rows = state_ref.shape[0] * HEAD_COUNT

    @pl.when(step == 0)
    def _():
        for number, source in enumerate((const0, const1, const2, const3)):
            pair = source[...]
            turned = pltpu.roll(pair, HEAD_SIZE, 1)
            first = lax.broadcasted_iota(jnp.int32, pair.shape, 1) < HEAD_SIZE
            count = pair.shape[0]
            consts_ref[number, pl.ds(0, count, stride=2), :] = jnp.where(first, pair, turned)
            consts_ref[number, pl.ds(1, count, stride=2), :] = jnp.where(first, turned, pair)
        for head in range(HEAD_COUNT):
            total = dot(land_ref[head * pieces], place_ref[0])
            for piece in range(1, pieces):
                total = total + dot(land_ref[head * pieces + piece], place_ref[piece])
            for number in range(ROLES):
                part = total[:, number * LANES : (number + 1) * LANES]
                role_ref[number, pl.ds(head, tokens, stride=HEAD_COUNT), :] = part

    base = pl.multiple_of(step * step_rows, step_rows)

    def role(number):
        return role_ref[number, pl.ds(base, step_rows), :]

    def const(number):
        one = consts_ref[number]
        return jnp.concatenate([one] * state_ref.shape[0], axis=0)

    half = HEAD_SIZE / LANES

    def head_sum(value):
        return jnp.sum(value, axis=-1, keepdims=True) * half

    receptance, keys, values = role(0), role(1), role(2)
    decay = jnp.exp(-math.exp(-0.5) * jax.nn.sigmoid(const(0) + role(3)))
    rate = jax.nn.sigmoid(const(1) + role(4))
    unit_key = keys * lax.rsqrt(1.0 + head_sum(keys * keys))
    scaled_key = keys * rate
    removal = unit_key * rate
    self_sum = head_sum(receptance * scaled_key * const(2))

    def twice(value):
        return jnp.concatenate([value, value], axis=1)

    unit_key2, decay2, removal2 = twice(unit_key), twice(decay), twice(removal)
    scaled_key2, receptance2 = twice(scaled_key), twice(receptance)
    values_b = values[:, :HEAD_SIZE].astype(BF16)
    block = block_ref[...]
    chunk = block.shape[0]
    read = jnp.zeros((step_rows, LANES), F32)
    group = state_ref.shape[0]
    for c in range(HEAD_SIZE * HEAD_SIZE // chunk):
        cols = slice(c * chunk, (c + 1) * chunk)
        state = state_ref[:, :, cols].reshape(step_rows, chunk)
        high, low = split(state * unit_key2)
        recalled = dot(high, block) + dot(low, block)
        spread = dot(values_b, spread_ref[:, cols])
        new = state * decay2 - recalled * removal2 + spread * scaled_key2
        next_ref[:, :, cols] = new.reshape(group, HEAD_COUNT, chunk)
        high, low = split(new * receptance2)
        pick = gather_ref[cols, :]
        read = read + dot(high, pick) + dot(low, pick)
    centered = read - head_sum(read) * (1.0 / HEAD_SIZE)
    variance = head_sum(centered * centered) * (1.0 / HEAD_SIZE)
    normal = centered * lax.rsqrt(variance + 0.00064) * const(3)
    mixed_ref[pl.ds(base, step_rows), :] = (normal + self_sum * values) * jax.nn.sigmoid(role(5))

    @pl.when(step == pl.num_programs(0) - 1)
    def _():
        lane = lax.broadcasted_iota(jnp.int32, (tokens, LANES), 1)
        per = LANES // HEAD_SIZE
        parts = []
        for first in range(0, HEAD_COUNT, per):
            part = mixed_ref[pl.ds(first, tokens, stride=HEAD_COUNT), :]
            for other in range(1, per):
                rest = mixed_ref[pl.ds(first + other, tokens, stride=HEAD_COUNT), :]
                part = jnp.where(lane < other * HEAD_SIZE, part, rest)
            parts.append(part.astype(BF16))
        mixed = jnp.concatenate(parts, axis=1)
        attended = dot(mixed, out_w_ref[...]).astype(BF16).astype(F32)
        middle = resid_ref[...].astype(F32) + attended
        middle_ref[...] = middle
        normed = rms_norm(middle, gain_ref[...])
        normed_ref[...] = normed
        rows_ref[...] = dot(select_ref[...], normed).reshape(rows_ref.shape).astype(BF16)


def mixer(land, consts, state, out_w, resid, gain, select):
    sources, tokens, width = land.shape
    pieces = sources // HEAD_COUNT
    model = resid.shape[1]
    group = 8 if tokens % 8 == 0 else 1
    chunk = 4 * HEAD_SIZE
    place = jnp.asarray(place_matrices(pieces), BF16)
    eye = np.eye(HEAD_SIZE, dtype=np.float32)
    spread = jnp.asarray(np.repeat(eye, HEAD_SIZE, axis=1), BF16)
    gather = jnp.asarray(np.repeat(np.concatenate([eye] * (LANES // HEAD_SIZE), 1), HEAD_SIZE, 0), BF16)
    block = jnp.asarray(np.kron(np.eye(chunk // HEAD_SIZE), np.ones((HEAD_SIZE, HEAD_SIZE))), BF16)
    full = lambda array: pl.BlockSpec(array.shape, lambda i: (0,) * array.ndim)
    state_spec = pl.BlockSpec((group,) + state.shape[1:], lambda i: (i, 0, 0))
    operands = (land, place, spread, gather, block, *consts, state, out_w, resid, gain, select)
    specs = [full(a) for a in operands]
    specs[9] = state_spec
    whole = lambda shape: pl.BlockSpec(shape, lambda i: (0,) * len(shape))
    slots = select.shape[0]
    return pl.pallas_call(
        mixer_kernel,
        grid=(tokens // group,),
        out_shape=(
            jax.ShapeDtypeStruct(state.shape, F32),
            jax.ShapeDtypeStruct((tokens, model), F32),
            jax.ShapeDtypeStruct((tokens, model), BF16),
            jax.ShapeDtypeStruct((slots // CAP, CAP, model), BF16),
        ),
        in_specs=specs,
        out_specs=(state_spec, whole((tokens, model)), whole((tokens, model)), whole((slots // CAP, CAP, model))),
        scratch_shapes=[
            pltpu.VMEM((ROLES, tokens * HEAD_COUNT, LANES), F32),
            pltpu.VMEM((tokens * HEAD_COUNT, LANES), F32),
            pltpu.VMEM((4, HEAD_COUNT, LANES), F32),
        ],
        compiler_params=pltpu.CompilerParams(vmem_limit_bytes=50 * 1024 * 1024),
        cost_estimate=pl.CostEstimate(flops=4_000_000_000, bytes_accessed=20_000_000, transcendentals=0),
    )(*operands)


PLANE = 8


def project_kernel(
    depth, normed_ref, w0, w1, w2, w3, w4, w5, land_out,
    weight_ref, held, cols, land,
    z_send, z_recv, near_send, near_recv, half_send, half_recv, core_send, core_recv,
    out_send, out_recv,
):
    total = depth * PLANE
    tokens, model = normed_ref.shape
    cut = model // 2
    me = lax.axis_index("ep")
    core = lax.rem(me, 2)
    x = lax.rem(me // 2, 2)
    y = lax.rem(me // 4, 2)
    along_x = me + 2 - 4 * x
    along_y = me + 4 - 8 * y
    mate = me + 1 - 2 * core
    plane = lax.rem(me, PLANE)
    plane_x, plane_y, plane_c = lax.rem(along_x, PLANE), lax.rem(along_y, PLANE), lax.rem(mate, PLANE)
    far = lax.rem(along_x + 4 - 8 * y, PLANE)
    level = me // PLANE

    def send(source, target, device, send_sem, recv_sem):
        copy = pltpu.make_async_remote_copy(
            src_ref=source, dst_ref=target, send_sem=send_sem, recv_sem=recv_sem,
            device_id={"ep": device}, device_id_type=pl.DeviceIdType.MESH,
        )
        copy.start()
        return copy

    def slot(of_plane, d):
        return held.at[of_plane, lax.rem(level + depth - d, depth)]

    sent = []
    along_z = [None]
    for d in range(1, depth):
        there = lax.rem(me + PLANE * d, total)
        along_z.append(send(normed_ref, slot(plane, 0), there, z_send.at[d], z_recv.at[d]))
    by_y, by_x, by_core = [], [], [[], [], [], []]
    for d in range(depth):
        if d:
            along_z[d].wait_recv()
        source = normed_ref if d == 0 else slot(plane, d)
        here = slot(plane, d)
        by_y.append(send(source, here, along_y, near_send.at[0, d], near_recv.at[0, d]))
        by_x.append(send(source, here, along_x, near_send.at[1, d], near_recv.at[1, d]))
        by_core[0].append(send(source, here, mate, core_send.at[0, d], core_recv.at[0, d]))
        if d == 0:
            held[plane, level] = normed_ref[...]
            weight_ref[...] = jnp.concatenate(
                [w[...] for w in (w0, w1, w2, w3, w4, w5)], axis=0
            )

    def compute(group):
        rows = held[group].astype(F32).reshape(depth * tokens, model).astype(BF16)
        result = lax.dot_general(
            rows, weight_ref[...], (((1,), (1,)), ((), ())), preferred_element_type=F32
        )
        cols[group] = result.reshape(depth, tokens, result.shape[-1]).astype(BF16)

    def give(group):
        for z in range(depth):
            to = z * PLANE + group
            number = lax.rem(to - me + total, total)

            @pl.when(to != me)
            def _():
                send(cols.at[group, z], land.at[me], to, out_send.at[number], out_recv.at[number])

            @pl.when(to == me)
            def _():
                land[me] = cols[group, z]

    compute(plane)
    halves = []
    for d in range(depth):
        by_y[d].wait_recv()
        block = held.at[plane_y, lax.rem(level + depth - d, depth)]
        first = block.at[:, :cut]
        halves.append(send(first, first, along_x, half_send.at[0, d], half_recv.at[0, d]))
        by_core[1].append(send(block, block, mate, core_send.at[1, d], core_recv.at[1, d]))
        by_x[d].wait_recv()
        block = held.at[plane_x, lax.rem(level + depth - d, depth)]
        second = block.at[:, cut:]
        halves.append(send(second, second, along_y, half_send.at[1, d], half_recv.at[1, d]))
        by_core[2].append(send(block, block, mate, core_send.at[2, d], core_recv.at[2, d]))
    compute(plane_y)
    give(plane)
    compute(plane_x)
    give(plane_y)
    for d in range(depth):
        halves[2 * d].wait_recv()
        halves[2 * d + 1].wait_recv()
        block = slot(far, d)
        by_core[3].append(send(block, block, mate, core_send.at[3, d], core_recv.at[3, d]))
    before = plane_x
    compute(far)
    give(before)
    before = far
    for which, group in enumerate((plane, plane_y, plane_x, far)):
        for d in range(depth):
            by_core[which][d].wait_recv()
        other = group + 1 - 2 * core
        compute(other)
        give(before)
        before = other
    give(before)
    for copy in along_z[1:] + by_y + by_x + halves + by_core[0] + by_core[1] + by_core[2] + by_core[3]:
        copy.wait_send()

    def finish(number, carry):
        copy = pltpu.make_async_remote_copy(
            src_ref=cols.at[0, 0], dst_ref=land.at[0],
            send_sem=out_send.at[number], recv_sem=out_recv.at[number],
            device_id={"ep": lax.rem(me + number, total)}, device_id_type=pl.DeviceIdType.MESH,
        )
        copy.wait_recv()
        copy.wait_send()
        return carry

    lax.fori_loop(1, total, finish, 0)
    land_out[...] = land[...]


def project(normed, weights, ep_size):
    depth = ep_size // PLANE
    tokens, model = normed.shape
    weights = [w.T for w in weights]
    width = sum(w.shape[0] for w in weights)
    dma = pltpu.SemaphoreType.DMA
    return pl.pallas_call(
        functools.partial(project_kernel, depth),
        out_shape=jax.ShapeDtypeStruct((ep_size, tokens, width), BF16),
        in_specs=[pl.BlockSpec(memory_space=pltpu.VMEM)] * 7,
        out_specs=pl.BlockSpec(memory_space=pltpu.VMEM),
        scratch_shapes=[
            pltpu.VMEM((width, model), BF16),
            pltpu.VMEM((PLANE, depth, tokens, model), BF16),
            pltpu.VMEM((PLANE, depth, tokens, width), BF16),
            pltpu.VMEM((ep_size, tokens, width), BF16),
            dma((depth,)), dma((depth,)),
            dma((2, depth)), dma((2, depth)),
            dma((2, depth)), dma((2, depth)),
            dma((4, depth)), dma((4, depth)),
            dma((ep_size,)), dma((ep_size,)),
        ],
        compiler_params=pltpu.CompilerParams(
            has_side_effects=True, vmem_limit_bytes=40 * 1024 * 1024
        ),
        cost_estimate=pl.CostEstimate(flops=600_000_000, bytes_accessed=100_000_000, transcendentals=0),
    )(normed, *weights)


def experts_kernel(
    depth, rows_ref, normed_ref, middle_ref, coef_ref, g0, g1, g2, g3, g4, g5, out_ref,
    b0, b1, b2, b3, b4, b5, served, output, returned,
    load_sem, go_send, go_recv, back_send, back_recv,
):
    total = depth * PLANE
    tokens, model = normed_ref.shape
    me = lax.axis_index("ep")
    level = me // PLANE

    def copy_of(source, target, device, send_sem, recv_sem):
        return pltpu.make_async_remote_copy(
            src_ref=source, dst_ref=target, send_sem=send_sem, recv_sem=recv_sem,
            device_id={"ep": device}, device_id_type=pl.DeviceIdType.MESH,
        )

    def go(number):
        to = lax.rem(me + number, total)
        return copy_of(rows_ref.at[to], served.at[me], to, go_send.at[number], go_recv.at[number])

    def back(to):
        number = lax.rem(to - me + total, total)
        return copy_of(
            output.at[to], returned.at[me], to, back_send.at[number], back_recv.at[number]
        )

    def launch(number, carry):
        go(number).start()
        return carry

    lax.fori_loop(1, total, launch, 0)
    loads = [
        pltpu.make_async_copy(source, target, load_sem.at[i])
        for i, (source, target) in enumerate(zip((g0, g1, g2, g3, g4, g5), (b0, b1, b2, b3, b4, b5)))
    ]
    for load in loads:
        load.start()
    served[me] = rows_ref[me]
    for load in loads[:3]:
        load.wait()
    shared = expert_mlp(normed_ref[...], b0[...], b1[...], b2[...])
    partial = middle_ref[...] + shared.astype(F32)
    for load in loads[3:]:
        load.wait()

    for d in range(depth):
        first = lax.rem(level + depth - d, depth) * PLANE

        def arrive(i, carry):
            source = first + i

            @pl.when(source != me)
            def _():
                go(lax.rem(me - source + total, total)).wait_recv()

            return carry

        lax.fori_loop(0, PLANE, arrive, 0)
        rows = served[pl.ds(first, PLANE)].reshape(PLANE * CAP, model)
        result = expert_mlp(rows, b3[...], b4[...], b5[...])
        output[pl.ds(first, PLANE)] = result.reshape(PLANE, CAP, model)

        def give(i, carry):
            source = first + i

            @pl.when(source != me)
            def _():
                back(source).start()

            return carry

        lax.fori_loop(0, PLANE, give, 0)
    returned[me] = output[me]

    def finish(number, carry):
        go(number).wait_send()
        ended = back(lax.rem(me + number, total))
        ended.wait_recv()
        ended.wait_send()
        return carry

    lax.fori_loop(1, total, finish, 0)
    routed = dot(coef_ref[...], returned[...].reshape(total * CAP, model))
    out_ref[...] = (partial + (routed[:tokens] + routed[tokens:])).astype(BF16)


def experts_step(rows, normed, middle, coef, weights, ep_size):
    depth = ep_size // PLANE
    tokens, model = normed.shape
    dma = pltpu.SemaphoreType.DMA
    vmem = pl.BlockSpec(memory_space=pltpu.VMEM)
    return pl.pallas_call(
        functools.partial(experts_kernel, depth),
        out_shape=jax.ShapeDtypeStruct((tokens, model), BF16),
        in_specs=[vmem] * 4 + [pl.BlockSpec(memory_space=pl.ANY)] * 6,
        out_specs=vmem,
        scratch_shapes=[pltpu.VMEM(w.shape, BF16) for w in weights]
        + [pltpu.VMEM(rows.shape, BF16)] * 3
        + [dma((6,))]
        + [dma((ep_size,))] * 4,
        compiler_params=pltpu.CompilerParams(
            has_side_effects=True, vmem_limit_bytes=40 * 1024 * 1024
        ),
        cost_estimate=pl.CostEstimate(flops=1_000_000_000, bytes_accessed=60_000_000, transcendentals=0),
    )(rows, normed, middle, coef, *weights)


def per_device(
    residual_input,
    attention_norm_gain,
    receptance_weight,
    key_weight,
    value_weight,
    decay_weight,
    correction_rate_weight,
    output_gate_weight,
    decay_offset,
    correction_rate_offset,
    self_term_weight,
    head_read_gain,
    previous_state,
    attention_output_weight,
    feedforward_norm_gain,
    routes,
    routing_weight,
    routed_gate_weight,
    routed_up_weight,
    routed_down_weight,
    common_gate_weight,
    common_up_weight,
    common_down_weight,
):
    ep_size = lax.axis_size("ep")
    device = lax.axis_index("ep")
    tokens, model = residual_input.shape
    normed = rms_norm(residual_input.astype(F32), attention_norm_gain)
    own_routes = lax.dynamic_slice_in_dim(routes, device * tokens, tokens, 0)
    own_weight = lax.dynamic_slice_in_dim(routing_weight, device * tokens, tokens, 0)
    experts = routed_gate_weight.shape[0] * ep_size
    match = own_routes[:, :, None] == jnp.arange(experts, dtype=jnp.int32)
    hit = jnp.any(match, axis=1)
    weight = jnp.sum(jnp.where(match, own_weight[:, :, None], 0.0), axis=1)
    rank = jnp.cumsum(hit.astype(jnp.int32), axis=0) - hit.astype(jnp.int32)
    chosen = hit[:, :, None] & (rank[:, :, None] == jnp.arange(CAP, dtype=jnp.int32))
    select = chosen.astype(BF16).reshape(tokens, experts * CAP)
    coefficient = jnp.where(chosen, weight[:, :, None], 0.0).reshape(tokens, experts * CAP)
    coef_high, coef_low = split(coefficient)

    land = project(
        normed,
        (
            receptance_weight,
            key_weight,
            value_weight,
            decay_weight,
            correction_rate_weight,
            output_gate_weight,
        ),
        ep_size,
    )
    consts = [
        c.reshape(-1, LANES)
        for c in (decay_offset, correction_rate_offset, self_term_weight, head_read_gain)
    ]
    next_state, middle, normed_ffn, rows = mixer(
        land,
        consts,
        previous_state,
        attention_output_weight,
        residual_input,
        feedforward_norm_gain.reshape(1, model),
        select.T,
    )
    hidden_out = experts_step(
        rows,
        normed_ffn,
        middle,
        jnp.concatenate((coef_high, coef_low), axis=0),
        (
            common_gate_weight,
            common_up_weight,
            common_down_weight,
            routed_gate_weight[0],
            routed_up_weight[0],
            routed_down_weight[0],
        ),
        ep_size,
    )
    return (hidden_out, next_state)


def solution(mesh):
    return jax.shard_map(
        per_device,
        mesh=mesh,
        in_specs=(
            P(("grp", "ep"), None),
            P(),
            P(None, "ep"),
            P(None, "ep"),
            P(None, "ep"),
            P(None, "ep"),
            P(None, "ep"),
            P(None, "ep"),
            P(),
            P(),
            P(),
            P(),
            P(("grp", "ep"), None, None),
            P(),
            P(),
            P("grp", None),
            P("grp", None),
            P("ep", None, None),
            P("ep", None, None),
            P("ep", None, None),
            P(),
            P(),
            P(),
        ),
        out_specs=(P(("grp", "ep"), None), P(("grp", "ep"), None, None)),
        check_vma=False,
    )
```

```python
import functools
import math

import jax
import jax.numpy as jnp
import numpy as np
from jax import lax
from jax.experimental import pallas as pl
from jax.experimental.pallas import tpu as pltpu
from jax.sharding import PartitionSpec as P

HEAD_COUNT = 16
HEAD_SIZE = 64
CAP = 4
ROLES = 6
LANES = 128
F32 = jnp.float32
BF16 = jnp.bfloat16


def rms_norm(value_rows, gain):
    scale = lax.rsqrt(jnp.mean(value_rows * value_rows, axis=-1, keepdims=True) + 1e-06)
    return (value_rows * scale * gain.astype(F32)).astype(BF16)


def expert_mlp(rows, gate_w, up_w, down_w):
    gate = jnp.dot(rows, gate_w, preferred_element_type=F32)
    upward = jnp.dot(rows, up_w, preferred_element_type=F32)
    hidden = (jax.nn.silu(gate) * upward).astype(BF16)
    return jnp.dot(hidden, down_w, preferred_element_type=F32).astype(BF16)


def place_matrices(pieces):
    width = HEAD_SIZE // pieces
    place = np.zeros((pieces, ROLES * width, ROLES * LANES), np.float32)
    for piece in range(pieces):
        for role in range(ROLES):
            for column in range(width):
                for copy in range(LANES // HEAD_SIZE):
                    lane = role * LANES + copy * HEAD_SIZE + piece * width + column
                    place[piece, role * width + column, lane] = 1.0
    return place


def split(value):
    high = value.astype(BF16)
    return high, (value - high.astype(F32)).astype(BF16)


def dot(a, b):
    return jnp.dot(a, b, preferred_element_type=F32)


def mixer_kernel(
    land_ref, place_ref, spread_ref, gather_ref, block_ref, const0, const1, const2, const3, state_ref, out_w_ref,
    resid_ref, gain_ref, select_ref,
    next_ref, middle_ref, normed_ref, rows_ref,
    role_ref, mixed_ref, consts_ref,
):
    step = pl.program_id(0)
    tokens = land_ref.shape[1]
    pieces = place_ref.shape[0]
    step_rows = state_ref.shape[0] * HEAD_COUNT

    @pl.when(step == 0)
    def _():
        for number, source in enumerate((const0, const1, const2, const3)):
            pair = source[...]
            turned = pltpu.roll(pair, HEAD_SIZE, 1)
            first = lax.broadcasted_iota(jnp.int32, pair.shape, 1) < HEAD_SIZE
            count = pair.shape[0]
            consts_ref[number, pl.ds(0, count, stride=2), :] = jnp.where(first, pair, turned)
            consts_ref[number, pl.ds(1, count, stride=2), :] = jnp.where(first, turned, pair)
        for head in range(HEAD_COUNT):
            total = dot(land_ref[head * pieces], place_ref[0])
            for piece in range(1, pieces):
                total = total + dot(land_ref[head * pieces + piece], place_ref[piece])
            for number in range(ROLES):
                part = total[:, number * LANES : (number + 1) * LANES]
                role_ref[number, pl.ds(head, tokens, stride=HEAD_COUNT), :] = part

    base = pl.multiple_of(step * step_rows, step_rows)

    def role(number):
        return role_ref[number, pl.ds(base, step_rows), :]

    def const(number):
        one = consts_ref[number]
        return jnp.concatenate([one] * state_ref.shape[0], axis=0)

    half = HEAD_SIZE / LANES

    def head_sum(value):
        return jnp.sum(value, axis=-1, keepdims=True) * half

    receptance, keys, values = role(0), role(1), role(2)
    decay = jnp.exp(-math.exp(-0.5) * jax.nn.sigmoid(const(0) + role(3)))
    rate = jax.nn.sigmoid(const(1) + role(4))
    unit_key = keys * lax.rsqrt(1.0 + head_sum(keys * keys))
    scaled_key = keys * rate
    removal = unit_key * rate
    self_sum = head_sum(receptance * scaled_key * const(2))

    def twice(value):
        return jnp.concatenate([value, value], axis=1)

    unit_key2, decay2, removal2 = twice(unit_key), twice(decay), twice(removal)
    scaled_key2, receptance2 = twice(scaled_key), twice(receptance)
    values_b = values[:, :HEAD_SIZE].astype(BF16)
    block = block_ref[...]
    chunk = block.shape[0]
    read = jnp.zeros((step_rows, LANES), F32)
    group = state_ref.shape[0]
    for c in range(HEAD_SIZE * HEAD_SIZE // chunk):
        cols = slice(c * chunk, (c + 1) * chunk)
        state = state_ref[:, :, cols].reshape(step_rows, chunk)
        high, low = split(state * unit_key2)
        recalled = dot(high, block) + dot(low, block)
        spread = dot(values_b, spread_ref[:, cols])
        new = state * decay2 - recalled * removal2 + spread * scaled_key2
        next_ref[:, :, cols] = new.reshape(group, HEAD_COUNT, chunk)
        high, low = split(new * receptance2)
        pick = gather_ref[cols, :]
        read = read + dot(high, pick) + dot(low, pick)
    centered = read - head_sum(read) * (1.0 / HEAD_SIZE)
    variance = head_sum(centered * centered) * (1.0 / HEAD_SIZE)
    normal = centered * lax.rsqrt(variance + 0.00064) * const(3)
    mixed_ref[pl.ds(base, step_rows), :] = (normal + self_sum * values) * jax.nn.sigmoid(role(5))

    @pl.when(step == pl.num_programs(0) - 1)
    def _():
        lane = lax.broadcasted_iota(jnp.int32, (tokens, LANES), 1)
        per = LANES // HEAD_SIZE
        parts = []
        for first in range(0, HEAD_COUNT, per):
            part = mixed_ref[pl.ds(first, tokens, stride=HEAD_COUNT), :]
            for other in range(1, per):
                rest = mixed_ref[pl.ds(first + other, tokens, stride=HEAD_COUNT), :]
                part = jnp.where(lane < other * HEAD_SIZE, part, rest)
            parts.append(part.astype(BF16))
        mixed = jnp.concatenate(parts, axis=1)
        attended = dot(mixed, out_w_ref[...]).astype(BF16).astype(F32)
        middle = resid_ref[...].astype(F32) + attended
        middle_ref[...] = middle
        normed = rms_norm(middle, gain_ref[...])
        normed_ref[...] = normed
        rows_ref[...] = dot(select_ref[...], normed).reshape(rows_ref.shape).astype(BF16)


def mixer(land, consts, state, out_w, resid, gain, select):
    sources, tokens, width = land.shape
    pieces = sources // HEAD_COUNT
    model = resid.shape[1]
    group = 8 if tokens % 8 == 0 else 1
    chunk = 4 * HEAD_SIZE
    place = jnp.asarray(place_matrices(pieces), BF16)
    eye = np.eye(HEAD_SIZE, dtype=np.float32)
    spread = jnp.asarray(np.repeat(eye, HEAD_SIZE, axis=1), BF16)
    gather = jnp.asarray(np.repeat(np.concatenate([eye] * (LANES // HEAD_SIZE), 1), HEAD_SIZE, 0), BF16)
    block = jnp.asarray(np.kron(np.eye(chunk // HEAD_SIZE), np.ones((HEAD_SIZE, HEAD_SIZE))), BF16)
    full = lambda array: pl.BlockSpec(array.shape, lambda i: (0,) * array.ndim)
    state_spec = pl.BlockSpec((group,) + state.shape[1:], lambda i: (i, 0, 0))
    operands = (land, place, spread, gather, block, *consts, state, out_w, resid, gain, select)
    specs = [full(a) for a in operands]
    specs[9] = state_spec
    whole = lambda shape: pl.BlockSpec(shape, lambda i: (0,) * len(shape))
    slots = select.shape[0]
    return pl.pallas_call(
        mixer_kernel,
        grid=(tokens // group,),
        out_shape=(
            jax.ShapeDtypeStruct(state.shape, F32),
            jax.ShapeDtypeStruct((tokens, model), F32),
            jax.ShapeDtypeStruct((tokens, model), BF16),
            jax.ShapeDtypeStruct((slots // CAP, CAP, model), BF16),
        ),
        in_specs=specs,
        out_specs=(state_spec, whole((tokens, model)), whole((tokens, model)), whole((slots // CAP, CAP, model))),
        scratch_shapes=[
            pltpu.VMEM((ROLES, tokens * HEAD_COUNT, LANES), F32),
            pltpu.VMEM((tokens * HEAD_COUNT, LANES), F32),
            pltpu.VMEM((4, HEAD_COUNT, LANES), F32),
        ],
        compiler_params=pltpu.CompilerParams(vmem_limit_bytes=50 * 1024 * 1024),
        cost_estimate=pl.CostEstimate(flops=4_000_000_000, bytes_accessed=20_000_000, transcendentals=0),
    )(*operands)


PLANE = 8


def project_kernel(
    depth, normed_ref, w0, w1, w2, w3, w4, w5, land_out,
    weight_ref, held, cols, land,
    z_send, z_recv, near_send, near_recv, half_send, half_recv, core_send, core_recv,
    out_send, out_recv, load_sem,
):
    total = depth * PLANE
    tokens, model = normed_ref.shape
    cut = model // 2
    me = lax.axis_index("ep")
    core = lax.rem(me, 2)
    x = lax.rem(me // 2, 2)
    y = lax.rem(me // 4, 2)
    along_x = me + 2 - 4 * x
    along_y = me + 4 - 8 * y
    mate = me + 1 - 2 * core
    plane = lax.rem(me, PLANE)
    plane_x, plane_y, plane_c = lax.rem(along_x, PLANE), lax.rem(along_y, PLANE), lax.rem(mate, PLANE)
    far = lax.rem(along_x + 4 - 8 * y, PLANE)
    level = me // PLANE

    def send(source, target, device, send_sem, recv_sem):
        copy = pltpu.make_async_remote_copy(
            src_ref=source, dst_ref=target, send_sem=send_sem, recv_sem=recv_sem,
            device_id={"ep": device}, device_id_type=pl.DeviceIdType.MESH,
        )
        copy.start()
        return copy

    def slot(of_plane, d):
        return held.at[of_plane, lax.rem(level + depth - d, depth)]

    loads = []
    for i, w in enumerate((w0, w1, w2, w3, w4, w5)):
        part = weight_ref.at[pl.ds(i * w.shape[0], w.shape[0])]
        loads.append(pltpu.make_async_copy(w, part, load_sem.at[i]))
        loads[-1].start()
    along_z = [None]
    for d in range(1, depth):
        there = lax.rem(me + PLANE * d, total)
        along_z.append(send(normed_ref, slot(plane, 0), there, z_send.at[d], z_recv.at[d]))
    by_y, by_x, by_core = [], [], [[], [], [], []]
    for d in range(depth):
        if d:
            along_z[d].wait_recv()
        source = normed_ref if d == 0 else slot(plane, d)
        here = slot(plane, d)
        by_y.append(send(source, here, along_y, near_send.at[0, d], near_recv.at[0, d]))
        by_x.append(send(source, here, along_x, near_send.at[1, d], near_recv.at[1, d]))
        by_core[0].append(send(source, here, mate, core_send.at[0, d], core_recv.at[0, d]))
        if d == 0:
            held[plane, level] = normed_ref[...]
            for load in loads:
                load.wait()

    def compute(group):
        rows = held[group].astype(F32).reshape(depth * tokens, model).astype(BF16)
        result = lax.dot_general(
            rows, weight_ref[...], (((1,), (1,)), ((), ())), preferred_element_type=F32
        )
        cols[group] = result.reshape(depth, tokens, result.shape[-1]).astype(BF16)

    def give(group):
        for z in range(depth):
            to = z * PLANE + group
            number = lax.rem(to - me + total, total)

            @pl.when(to != me)
            def _():
                send(cols.at[group, z], land.at[me], to, out_send.at[number], out_recv.at[number])

            @pl.when(to == me)
            def _():
                land[me] = cols[group, z]

    compute(plane)
    halves = []
    for d in range(depth):
        by_y[d].wait_recv()
        block = held.at[plane_y, lax.rem(level + depth - d, depth)]
        first = block.at[:, :cut]
        halves.append(send(first, first, along_x, half_send.at[0, d], half_recv.at[0, d]))
        by_core[1].append(send(block, block, mate, core_send.at[1, d], core_recv.at[1, d]))
        by_x[d].wait_recv()
        block = held.at[plane_x, lax.rem(level + depth - d, depth)]
        second = block.at[:, cut:]
        halves.append(send(second, second, along_y, half_send.at[1, d], half_recv.at[1, d]))
        by_core[2].append(send(block, block, mate, core_send.at[2, d], core_recv.at[2, d]))
    compute(plane_y)
    give(plane)
    compute(plane_x)
    give(plane_y)
    for d in range(depth):
        halves[2 * d].wait_recv()
        halves[2 * d + 1].wait_recv()
        block = slot(far, d)
        by_core[3].append(send(block, block, mate, core_send.at[3, d], core_recv.at[3, d]))
    before = plane_x
    compute(far)
    give(before)
    before = far
    for which, group in enumerate((plane, plane_y, plane_x, far)):
        for d in range(depth):
            by_core[which][d].wait_recv()
        other = group + 1 - 2 * core
        compute(other)
        give(before)
        before = other
    give(before)
    for copy in along_z[1:] + by_y + by_x + halves + by_core[0] + by_core[1] + by_core[2] + by_core[3]:
        copy.wait_send()

    def finish(number, carry):
        copy = pltpu.make_async_remote_copy(
            src_ref=cols.at[0, 0], dst_ref=land.at[0],
            send_sem=out_send.at[number], recv_sem=out_recv.at[number],
            device_id={"ep": lax.rem(me + number, total)}, device_id_type=pl.DeviceIdType.MESH,
        )
        copy.wait_recv()
        copy.wait_send()
        return carry

    lax.fori_loop(1, total, finish, 0)
    land_out[...] = land[...]


def project(normed, weights, ep_size):
    depth = ep_size // PLANE
    tokens, model = normed.shape
    weights = [w.T for w in weights]
    width = sum(w.shape[0] for w in weights)
    dma = pltpu.SemaphoreType.DMA
    return pl.pallas_call(
        functools.partial(project_kernel, depth),
        out_shape=jax.ShapeDtypeStruct((ep_size, tokens, width), BF16),
        in_specs=[pl.BlockSpec(memory_space=pltpu.VMEM)]
        + [pl.BlockSpec(memory_space=pltpu.HBM)] * len(weights),
        out_specs=pl.BlockSpec(memory_space=pltpu.VMEM),
        scratch_shapes=[
            pltpu.VMEM((width, model), BF16),
            pltpu.VMEM((PLANE, depth, tokens, model), BF16),
            pltpu.VMEM((PLANE, depth, tokens, width), BF16),
            pltpu.VMEM((ep_size, tokens, width), BF16),
            dma((depth,)), dma((depth,)),
            dma((2, depth)), dma((2, depth)),
            dma((2, depth)), dma((2, depth)),
            dma((4, depth)), dma((4, depth)),
            dma((ep_size,)), dma((ep_size,)), dma((len(weights),)),
        ],
        compiler_params=pltpu.CompilerParams(
            has_side_effects=True, vmem_limit_bytes=60 * 1024 * 1024
        ),
        cost_estimate=pl.CostEstimate(flops=600_000_000, bytes_accessed=100_000_000, transcendentals=0),
    )(normed, *weights)


def experts_kernel(
    depth, rows_ref, normed_ref, middle_ref, coef_ref, g0, g1, g2, g3, g4, g5, out_ref,
    b0, b1, b2, b3, b4, b5, served, output, returned,
    load_sem, go_send, go_recv, back_send, back_recv,
):
    total = depth * PLANE
    tokens, model = normed_ref.shape
    me = lax.axis_index("ep")
    level = me // PLANE

    def copy_of(source, target, device, send_sem, recv_sem):
        return pltpu.make_async_remote_copy(
            src_ref=source, dst_ref=target, send_sem=send_sem, recv_sem=recv_sem,
            device_id={"ep": device}, device_id_type=pl.DeviceIdType.MESH,
        )

    def go(number):
        to = lax.rem(me + number, total)
        return copy_of(rows_ref.at[to], served.at[me], to, go_send.at[number], go_recv.at[number])

    def back(to):
        number = lax.rem(to - me + total, total)
        return copy_of(
            output.at[to], returned.at[me], to, back_send.at[number], back_recv.at[number]
        )

    def launch(number, carry):
        go(number).start()
        return carry

    lax.fori_loop(1, total, launch, 0)
    loads = [
        pltpu.make_async_copy(source, target, load_sem.at[i])
        for i, (source, target) in enumerate(zip((g0, g1, g2, g3, g4, g5), (b0, b1, b2, b3, b4, b5)))
    ]
    for load in loads:
        load.start()
    served[me] = rows_ref[me]
    for load in loads[:3]:
        load.wait()
    shared = expert_mlp(normed_ref[...], b0[...], b1[...], b2[...])
    partial = middle_ref[...] + shared.astype(F32)
    for load in loads[3:]:
        load.wait()

    for d in range(depth):
        first = lax.rem(level + depth - d, depth) * PLANE

        def arrive(i, carry):
            source = first + i

            @pl.when(source != me)
            def _():
                go(lax.rem(me - source + total, total)).wait_recv()

            return carry

        lax.fori_loop(0, PLANE, arrive, 0)
        rows = served[pl.ds(first, PLANE)].reshape(PLANE * CAP, model)
        result = expert_mlp(rows, b3[...], b4[...], b5[...])
        output[pl.ds(first, PLANE)] = result.reshape(PLANE, CAP, model)

        def give(i, carry):
            source = first + i

            @pl.when(source != me)
            def _():
                back(source).start()

            return carry

        lax.fori_loop(0, PLANE, give, 0)
    returned[me] = output[me]

    def finish(number, carry):
        go(number).wait_send()
        ended = back(lax.rem(me + number, total))
        ended.wait_recv()
        ended.wait_send()
        return carry

    lax.fori_loop(1, total, finish, 0)
    routed = dot(coef_ref[...], returned[...].reshape(total * CAP, model))
    out_ref[...] = (partial + (routed[:tokens] + routed[tokens:])).astype(BF16)


def experts_step(rows, normed, middle, coef, weights, ep_size):
    depth = ep_size // PLANE
    tokens, model = normed.shape
    dma = pltpu.SemaphoreType.DMA
    vmem = pl.BlockSpec(memory_space=pltpu.VMEM)
    return pl.pallas_call(
        functools.partial(experts_kernel, depth),
        out_shape=jax.ShapeDtypeStruct((tokens, model), BF16),
        in_specs=[vmem] * 4 + [pl.BlockSpec(memory_space=pltpu.HBM)] * 6,
        out_specs=vmem,
        scratch_shapes=[pltpu.VMEM(w.shape, BF16) for w in weights]
        + [pltpu.VMEM(rows.shape, BF16)] * 3
        + [dma((6,))]
        + [dma((ep_size,))] * 4,
        compiler_params=pltpu.CompilerParams(
            has_side_effects=True, vmem_limit_bytes=60 * 1024 * 1024
        ),
        cost_estimate=pl.CostEstimate(flops=1_000_000_000, bytes_accessed=60_000_000, transcendentals=0),
    )(rows, normed, middle, coef, *weights)


def per_device(
    residual_input,
    attention_norm_gain,
    receptance_weight,
    key_weight,
    value_weight,
    decay_weight,
    correction_rate_weight,
    output_gate_weight,
    decay_offset,
    correction_rate_offset,
    self_term_weight,
    head_read_gain,
    previous_state,
    attention_output_weight,
    feedforward_norm_gain,
    routes,
    routing_weight,
    routed_gate_weight,
    routed_up_weight,
    routed_down_weight,
    common_gate_weight,
    common_up_weight,
    common_down_weight,
):
    ep_size = lax.axis_size("ep")
    device = lax.axis_index("ep")
    tokens, model = residual_input.shape
    normed = rms_norm(residual_input.astype(F32), attention_norm_gain)
    own_routes = lax.dynamic_slice_in_dim(routes, device * tokens, tokens, 0)
    own_weight = lax.dynamic_slice_in_dim(routing_weight, device * tokens, tokens, 0)
    experts = routed_gate_weight.shape[0] * ep_size
    match = own_routes[:, :, None] == jnp.arange(experts, dtype=jnp.int32)
    hit = jnp.any(match, axis=1)
    weight = jnp.sum(jnp.where(match, own_weight[:, :, None], 0.0), axis=1)
    rank = jnp.cumsum(hit.astype(jnp.int32), axis=0) - hit.astype(jnp.int32)
    chosen = hit[:, :, None] & (rank[:, :, None] == jnp.arange(CAP, dtype=jnp.int32))
    select = chosen.astype(BF16).reshape(tokens, experts * CAP)
    coefficient = jnp.where(chosen, weight[:, :, None], 0.0).reshape(tokens, experts * CAP)
    coef_high, coef_low = split(coefficient)

    land = project(
        normed,
        (
            receptance_weight,
            key_weight,
            value_weight,
            decay_weight,
            correction_rate_weight,
            output_gate_weight,
        ),
        ep_size,
    )
    consts = [
        c.reshape(-1, LANES)
        for c in (decay_offset, correction_rate_offset, self_term_weight, head_read_gain)
    ]
    next_state, middle, normed_ffn, rows = mixer(
        land,
        consts,
        previous_state,
        attention_output_weight,
        residual_input,
        feedforward_norm_gain.reshape(1, model),
        select.T,
    )
    hidden_out = experts_step(
        rows,
        normed_ffn,
        middle,
        jnp.concatenate((coef_high, coef_low), axis=0),
        (
            common_gate_weight,
            common_up_weight,
            common_down_weight,
            routed_gate_weight[0],
            routed_up_weight[0],
            routed_down_weight[0],
        ),
        ep_size,
    )
    return (hidden_out, next_state)


def solution(mesh):
    return jax.shard_map(
        per_device,
        mesh=mesh,
        in_specs=(
            P(("grp", "ep"), None),
            P(),
            P(None, "ep"),
            P(None, "ep"),
            P(None, "ep"),
            P(None, "ep"),
            P(None, "ep"),
            P(None, "ep"),
            P(),
            P(),
            P(),
            P(),
            P(("grp", "ep"), None, None),
            P(),
            P(),
            P("grp", None),
            P("grp", None),
            P("ep", None, None),
            P("ep", None, None),
            P("ep", None, None),
            P(),
            P(),
            P(),
        ),
        out_specs=(P(("grp", "ep"), None), P(("grp", "ep"), None, None)),
        check_vma=False,
    )
```
